32 devices in a mesh: ep: 8 (over z, x), tp: 4 (over y, core).
Axes of the slice: x: 2, y: 2, z: 4, core: 2. Of those that a mesh axis runs over, the one named last changes fastest.
Arguments:
- conv_value: bfloat16 [4096, 2048], P('ep', 'tp'), may hold values from -6 to 6
- conv_gate: bfloat16 [4096, 2048], P('ep', 'tp'), may hold values from -9 to 9
- conv_taps: float32 [31, 2048], P(None, 'tp'), may hold values from -14 to 14
- norm_gain: float32 [2048], P('tp'), may hold values from 0.1 to 1.9
- norm_shift: float32 [2048], P('tp'), may hold values from -3 to 3
- conv_out_weight: bfloat16 [2048, 2048], P(None, 'tp'), may hold values from -0.125 to 0.125
- moe_input: bfloat16 [1024, 2048], P('ep'), may hold values from -6 to 6
- moe_gain: float32 [2048], replicated, may hold values from 0.1 to 1.9
- routes: int32 [1024, 4], P('ep'), may hold values from 0 to 7, all different within a row; in each aligned block of 128 rows (0 to 127, 128 to 255, ...) at most 128 rows name the same one
- route_weights: float32 [1024, 4], P('ep'), may hold values from 0.25 to 1
- expert_gate: bfloat16 [8, 2048, 4096], P('ep', None, 'tp'), may hold values from -0.125 to 0.125
- expert_up: bfloat16 [8, 2048, 4096], P('ep', None, 'tp'), may hold values from -0.125 to 0.125
- expert_down: bfloat16 [8, 4096, 2048], P('ep', None, 'tp'), may hold values from -0.09375 to 0.09375
- shared_gate: bfloat16 [2048, 512], P(None, 'tp'), may hold values from -0.125 to 0.125
- shared_up: bfloat16 [2048, 512], P(None, 'tp'), may hold values from -0.125 to 0.125
- shared_down: bfloat16 [512, 2048], P(None, 'tp'), may hold values from -0.25 to 0.25
Outputs:
- conv_result: bfloat16 [4096, 2048], P('ep', 'tp')
- moe_result: bfloat16 [1024, 2048], P('ep', 'tp')
The draws below stay inside these ranges and needn't reach their ends.
Inputs may be any that keep to these rules, and one draw needn't show every extreme that they name: `routes`: in the rows of one device (aligned blocks of 128 rows) no expert is named by more than 128 rows, a bound that some block reaches; each row names 4 different experts.
All inputs are finite; a program needn't handle non-finite values.
Results may differ from the reference program's by a relative error of at most 0.0068.
Values may be sent and summed in bfloat16 or wider, within the bound.
A program may use at most 64 MiB of HBM per device.

```python
import math
import jax
import jax.numpy as jnp
import numpy as np
from jax import lax

D = 2048
FF = 4096
SHARED_FF = 512
CONV_WIDTH = 31
TOPK = 4
TOKB_DEV = 128
TOK_A = 4096
TOK_B = 1024
EXPERTS = 8
CAP = 128
N_EP = 8


def draw_conv_taps(key, part):
    base_key = jax.random.fold_in(key, 11)
    rough_key = jax.random.fold_in(key, 12)
    channel = jnp.arange(D, dtype=jnp.float32) / D
    base_draw = jnp.clip(jax.random.normal(base_key, (CONV_WIDTH, D), jnp.float32), -5.0, 5.0)
    channel_rise = jnp.exp(jnp.log(4.0) * channel)
    rough_scale = jax.random.uniform(rough_key, (D,), jnp.float32, 0.5, 1.5)
    return base_draw * channel_rise * rough_scale / jnp.sqrt(CONV_WIDTH * 1.0)


def block_scale(stream_key, shape, split, least, high):
    factor_of = 1.0
    for dim, blocks in split:
        draws = jax.random.uniform(jax.random.fold_in(jax.random.fold_in(stream_key, 6), dim), (blocks,), jnp.float32, least / len(split), high / len(split))
        factor_of = factor_of * jnp.repeat(jnp.exp(draws), shape[dim] // blocks).reshape((-1,) + (1,) * (len(shape) - 1 - dim))
    return factor_of


def routed_block(stream_key, own, number, rows, number_of, top, most, skew):
    order = jax.random.permutation(stream_key, number_of)
    packed, common = shares(number_of, rows * top, most, skew, True), shares(number_of, rows * top, most, skew, False)
    places = jnp.arange(number_of)

    def named(sizes, rotation):
        used = int((sizes > 0).sum())
        fixed = max(1, used // 4)
        shifted = fixed + (places - fixed + rotation * (used - fixed)) % max(1, number_of - fixed)
        return jnp.zeros((number_of,), jnp.int32).at[order[jnp.where(places < fixed, places, shifted)]].set(jnp.asarray(sizes, jnp.int32))

    sizes = jnp.where(number % 4 == 0, named(packed, number // 4), named(common, number - number // 4 - 1))
    mixed = jax.random.permutation(jax.random.fold_in(own, 3), number_of)
    giver, receiver = mixed[0:number_of // 2 * 2:2], mixed[1:number_of // 2 * 2:2]
    slack = jnp.minimum(sizes[giver] - 1, most - sizes[receiver]) // 2
    slack = jnp.where((giver == order[0]) | (receiver == order[0]) | (sizes[receiver] == 0), 0, jnp.maximum(slack, 0))
    shifted = jax.random.randint(jax.random.fold_in(own, 4), (number_of // 2,), 0, 1 << 20) % (slack + 1)
    sizes = sizes.at[giver].add(-shifted).at[receiver].add(shifted)
    items = jnp.searchsorted(jnp.cumsum(sizes), jnp.arange(rows * top), side="right").astype(jnp.int32)
    listing = items.reshape(top, rows).T
    listing = listing[jax.random.permutation(jax.random.fold_in(own, 1), rows)]
    rotation = jax.random.randint(jax.random.fold_in(own, 2), (rows, 1), 0, top)
    return jnp.take_along_axis(listing, (jnp.arange(top)[None, :] + rotation) % top, axis=1)


def shares(amount, total, reach, skew, full):
    portions = [(1 << 20) // math.isqrt(rank ** skew) + 1 for rank in range(1, amount + 1)]
    largest = reach if full else min(reach, max(-(-total // amount), total * portions[0] // sum(portions)))
    least = 1 if total - largest >= amount - 1 else 0
    given, surplus = [largest] + [least] * (amount - 1), total - largest - least * (amount - 1)
    while surplus > 0:
        movable = [i for i in range(1, amount) if given[i] < largest] or [i for i in range(1, amount) if given[i] < reach]
        whole, left = sum([portions[i] for i in movable]), surplus
        for i in movable:
            extra = min(reach - given[i], max(1, left * portions[i] // whole), surplus)
            given[i] = given[i] + extra
            surplus = surplus - extra
    return np.array(given)


def noise(rng, shape, width, reach, shards=(), kind=jnp.bfloat16):
    array = jax.random.normal(rng, shape, jnp.float32) * width
    if len(shards) > 0:
        array = block_scale(rng, shape, shards, -0.22, 0.18) * array
    return jnp.clip(array, min=-reach, max=reach).astype(kind)


def setup_inputs(seed: int = 0) -> dict:
    key_list = jax.random.split(jax.random.key(seed), 17)
    conv_value = noise(key_list[0], (TOK_A, D), 1.0, 6.0, ((0, 8), (1, 4)))
    conv_gate = noise(key_list[1], (TOK_A, D), 1.5, 9.0, ((0, 8), (1, 4)))
    conv_taps = draw_conv_taps(jax.random.fold_in(key_list[16], 71), 0)
    norm_gain = jnp.clip(1.0 + 0.18 * jax.random.normal(key_list[3], (D,), jnp.float32), 0.1, 1.9)
    norm_shift = noise(key_list[4], (D,), 0.5, 3.0, ((0, 4),), jnp.float32)
    conv_out_weight = noise(key_list[5], (D, D), D ** -0.5, 0.125, ((1, 4),))
    moe_input = noise(key_list[6], (TOK_B, D), 1.0, 6.0, ((0, 8),))
    moe_gain = jnp.clip(1.0 + 0.18 * jax.random.normal(key_list[7], (D,), jnp.float32), 0.1, 1.9)
    routes_keys = jax.random.split(jax.random.fold_in(key_list[8], 1), TOK_B // TOKB_DEV)
    routes_turns = jax.random.permutation(jax.random.fold_in(key_list[8], 3), TOK_B // TOKB_DEV)
    routes = jax.vmap(lambda own, number: routed_block(jax.random.fold_in(key_list[8], 2), own, number, TOKB_DEV, EXPERTS, TOPK, CAP, 2))(routes_keys, routes_turns).reshape((TOK_B, TOPK))
    route_weights = jnp.clip(0.25 + 0.75 * jax.random.uniform(key_list[9], (TOK_B, TOPK), jnp.float32) ** block_scale(key_list[9], (TOK_B, TOPK), ((0, 8),), -0.2, 0.2), 0.25, 1.0)
    expert_gate = noise(key_list[10], (EXPERTS, D, FF), D ** -0.5, 0.125, ((0, 8), (2, 4)))
    expert_up = noise(key_list[11], (EXPERTS, D, FF), D ** -0.5, 0.125, ((0, 8), (2, 4)))
    expert_down = noise(key_list[12], (EXPERTS, FF, D), FF ** -0.5, 0.09375, ((0, 8), (2, 4)))
    shared_gate = noise(key_list[13], (D, SHARED_FF), D ** -0.5, 0.125, ((1, 4),))
    shared_up = noise(key_list[14], (D, SHARED_FF), D ** -0.5, 0.125, ((1, 4),))
    shared_down = noise(key_list[15], (SHARED_FF, D), SHARED_FF ** -0.5, 0.25, ((1, 4),))
    return {"conv_value": conv_value, "conv_gate": conv_gate, "conv_taps": conv_taps, "norm_gain": norm_gain, "norm_shift": norm_shift, "conv_out_weight": conv_out_weight, "moe_input": moe_input, "moe_gain": moe_gain, "routes": routes, "route_weights": route_weights, "expert_gate": expert_gate, "expert_up": expert_up, "expert_down": expert_down, "shared_gate": shared_gate, "shared_up": shared_up, "shared_down": shared_down}


def reference(conv_value, conv_gate, conv_taps, norm_gain, norm_shift, conv_out_weight, moe_input, moe_gain, routes, route_weights, expert_gate, expert_up, expert_down, shared_gate, shared_up, shared_down):
    glu_rows = (conv_value.astype(jnp.float32) * jax.nn.sigmoid(conv_gate.astype(jnp.float32))).astype(jnp.bfloat16)
    padded = jnp.concatenate([jnp.zeros((CONV_WIDTH - 1, D), jnp.bfloat16), glu_rows], axis=0)
    filtered = jnp.zeros((TOK_A, D), jnp.float32)
    for offset in range(CONV_WIDTH):
        filtered = filtered + conv_taps[offset] * padded[offset:offset + TOK_A].astype(jnp.float32)
    row_mean = lax.optimization_barrier(jnp.mean(filtered, axis=1, keepdims=True))
    row_square = lax.optimization_barrier(jnp.mean(filtered * filtered, axis=1, keepdims=True))
    scaled = (filtered - row_mean) * lax.rsqrt(row_square - row_mean * row_mean + 1e-05)
    conv_hidden = jax.nn.silu(scaled * norm_gain + norm_shift).astype(jnp.bfloat16)
    conv_result = jnp.dot(conv_hidden, conv_out_weight, preferred_element_type=jnp.float32).astype(jnp.bfloat16)
    inputs = moe_input.astype(jnp.float32)
    normed = (inputs * lax.rsqrt(lax.optimization_barrier(jnp.mean(inputs * inputs, axis=1, keepdims=True)) + 1e-06) * moe_gain).astype(jnp.bfloat16)
    flat_expert = routes.reshape(-1).astype(jnp.int32)
    owner_row = (jnp.arange(TOK_B * TOPK, dtype=jnp.int32) // TOPK).astype(jnp.int32)
    sort_order = jnp.argsort(flat_expert, stable=True).astype(jnp.int32)
    sorted_owner = owner_row[sort_order]
    sorted_weight = route_weights.reshape(-1)[sort_order]
    counts = lax.optimization_barrier(jnp.sum((flat_expert[:, None] == jnp.arange(EXPERTS, dtype=jnp.int32)[None, :]).astype(jnp.int32), axis=0))
    starts = (jnp.cumsum(counts) - counts).astype(jnp.int32)
    slot_limit = N_EP * CAP
    pad_owner = jnp.concatenate([sorted_owner, jnp.zeros((slot_limit,), jnp.int32)])
    pad_weight = jnp.concatenate([sorted_weight, jnp.zeros((slot_limit,), jnp.float32)])

    def one_expert(running, expert_id):
        first_row = starts[expert_id]
        row_ids = lax.dynamic_slice_in_dim(pad_owner, first_row, slot_limit)
        weight = lax.dynamic_slice_in_dim(pad_weight, first_row, slot_limit)
        live_mask = (jnp.arange(slot_limit, dtype=jnp.int32) < counts[expert_id]).astype(jnp.float32)
        picked_rows = normed[row_ids]
        hidden = (jax.nn.silu(jnp.dot(picked_rows, expert_gate[expert_id], preferred_element_type=jnp.float32)) * jnp.dot(picked_rows, expert_up[expert_id], preferred_element_type=jnp.float32)).astype(jnp.bfloat16)
        expert_rows = jnp.dot(hidden, expert_down[expert_id], preferred_element_type=jnp.float32).astype(jnp.bfloat16)
        expert_rows = lax.optimization_barrier(expert_rows).astype(jnp.float32)
        return (running.at[row_ids].add(expert_rows * (weight * live_mask)[:, None]), None)
    routed, _ = lax.scan(one_expert, jnp.zeros((TOK_B, D), jnp.float32), jnp.arange(EXPERTS, dtype=jnp.int32))
    shared_hidden = (jax.nn.silu(jnp.dot(normed, shared_gate, preferred_element_type=jnp.float32)) * jnp.dot(normed, shared_up, preferred_element_type=jnp.float32)).astype(jnp.bfloat16)
    shared_sum = jnp.dot(shared_hidden, shared_down, preferred_element_type=jnp.float32)
    moe_result = (routed + shared_sum).astype(jnp.bfloat16)
    return (conv_result, moe_result)
```

```python
import functools

import jax
import jax.numpy as jnp
from jax import lax
from jax.experimental import pallas as pl
from jax.experimental.pallas import tpu as pltpu
from jax.sharding import PartitionSpec as P

MESH = pl.DeviceIdType.MESH
TILES = 2


def from_behind(value, axis, steps):
    count = lax.axis_size(axis)
    initial, last = (max(0, -steps), min(count, count - steps))
    return lax.ppermute(value, axis, [(source, source + steps) for source in range(initial, last)])


def silu(v):
    return v / (1.0 + jnp.exp(-v))


def moe_kernel(
    depth,
    normed,
    weights,
    gate_hbm,
    up_hbm,
    down_hbm,
    sgate,
    sup,
    sdown,
    out,
    gate,
    up,
    down,
    tokens,
    hidden,
    returned,
    outgoing,
    shidden,
    load_sem,
    own_sem,
    ssend,
    srecv,
    tsend,
    trecv,
    fsend,
    frecv,
    ysend,
    yrecv,
    psend,
    precv,
    gsend,
    grecv,
    rsend,
    rrecv,
):
    e = lax.axis_index("ep")
    q = lax.axis_index("tp")
    z, x = e // 2, e % 2
    y, c = q // 2, q % 2
    sister = (e, y * 2 + (1 - c))
    across = (e, (1 - y) * 2 + c)
    beside = (z * 2 + (1 - x), q)
    rows, width = normed.shape
    half = width // 2
    far = (1 - y) * 2 + c

    def home(s, a):
        return (((z + s) % depth) * 2 + (x if a == 0 else 1 - x), q)

    def copy(src, dst, send, recv, device):
        return pltpu.make_async_remote_copy(
            src_ref=src, dst_ref=dst, send_sem=send, recv_sem=recv, device_id=device, device_id_type=MESH
        )

    loads = [
        pltpu.make_async_copy(src.at[0], dst, load_sem.at[i])
        for i, (src, dst) in enumerate(((gate_hbm, gate), (up_hbm, up), (down_hbm, down)))
    ]
    for load in loads:
        load.start()
    own = [
        pltpu.make_async_copy(normed.at[:, h * half : (h + 1) * half], tokens.at[0, h, 0], own_sem.at[h])
        for h in range(2)
    ]
    for load in own:
        load.start()

    peers = [home(s, a) for s in range(depth) for a in range(2) if (s, a) != (0, 0)]
    peers += [(e, (q + k) % 4) for k in range(1, 4)]
    barrier = pltpu.get_barrier_semaphore()
    for peer in peers:
        pl.semaphore_signal(barrier, inc=1, device_id=peer, device_id_type=MESH)
    pl.semaphore_wait(barrier, len(peers))

    pending = []

    def launch(cp):
        cp.start()
        pending.append(cp)
        return cp

    for load in own:
        load.wait()
    mine = tokens.at[0, c, 0]
    arrive = {}
    arrive[0, 1] = launch(copy(mine, tokens.at[0, c, 1], tsend.at[0, 1], trecv.at[0, 1], beside))
    for s in range(1, depth):
        target = (((z + depth - s) % depth) * 2 + x, q)
        arrive[s, 0] = launch(copy(mine, tokens.at[s, c, 0], tsend.at[s, 0], trecv.at[s, 0], target))

    shared_gate = jnp.dot(normed[...], sgate[...], preferred_element_type=jnp.float32)
    shared_up = jnp.dot(normed[...], sup[...], preferred_element_type=jnp.float32)
    shidden[q] = (silu(shared_gate) * shared_up).astype(jnp.bfloat16)

    swapped = {}

    def pass_on(s, a):
        arrive[s, a].wait_recv()
        block = tokens.at[s, c, a]
        if a == 0:
            arrive[s, 1] = launch(copy(block, tokens.at[s, c, 1], tsend.at[s, 1], trecv.at[s, 1], beside))
        swapped[s, a] = launch(copy(block, tokens.at[s, c, a], fsend.at[s, a], frecv.at[s, a], sister))

    tile = hidden.shape[4]
    ycopies, pcopies = {}, {}

    def first(s):
        for t in range(TILES):
            cols = slice(t * tile, (t + 1) * tile)

            def product(weight):
                total = None
                for h in range(2):
                    block = tokens[s, h].reshape(2 * rows, half)
                    part = jnp.dot(block, weight[h * half : (h + 1) * half, cols], preferred_element_type=jnp.float32)
                    total = part if total is None else total + part
                return total

            hidden[s, q, t] = (silu(product(gate)) * product(up)).astype(jnp.bfloat16)
            block = hidden.at[s, q, t]
            ycopies[s, t] = launch(copy(block, hidden.at[s, q, t], ysend.at[s, t], yrecv.at[s, t], across))
            pcopies[s, t] = launch(copy(block, hidden.at[s, q, t], psend.at[s, t], precv.at[s, t], sister))

    pass_on(0, 1)
    pass_on(1, 0)
    swapped[0, 1].wait_recv()
    loads[0].wait()
    loads[1].wait()
    first(0)
    scopies = []
    for k in range(1, 4):
        scopies.append(
            launch(copy(shidden.at[q], shidden.at[q], ssend.at[k - 1], srecv.at[k - 1], (e, (q + k) % 4)))
        )
    for s in range(1, depth):
        if s + 1 < depth:
            pass_on(s + 1, 0)
        pass_on(s, 1)
        swapped[s, 0].wait_recv()
        swapped[s, 1].wait_recv()
        first(s)

    loads[2].wait()
    homes = {}
    for s in range(depth):
        forwards = []
        for t in range(TILES):
            ycopies[s, t].wait_recv()
            forwards.append(
                launch(copy(hidden.at[s, far, t], hidden.at[s, far, t], gsend.at[s, t], grecv.at[s, t], sister))
            )
            pcopies[s, t].wait_recv()
        for forward in forwards:
            forward.wait_recv()
        total = None
        for k in range(4):
            for t in range(TILES):
                at = (k * TILES + t) * tile
                part = jnp.dot(hidden[s, k, t], down[at : at + tile, :], preferred_element_type=jnp.float32)
                total = part if total is None else total + part
        for a in range(2):
            piece = total[a * rows : (a + 1) * rows].astype(jnp.bfloat16)
            if (s, a) == (0, 0):
                returned[0, 0] = piece
            else:
                outgoing[s, a] = piece
                homes[s, a] = launch(
                    copy(outgoing.at[s, a], returned.at[s, a], rsend.at[s, a], rrecv.at[s, a], home(s, a))
                )

    for cp in scopies:
        cp.wait_recv()
    moe_sum = None
    share = shidden.shape[2]
    for k in range(4):
        part = jnp.dot(shidden[k], sdown[k * share : (k + 1) * share, :], preferred_element_type=jnp.float32)
        moe_sum = part if moe_sum is None else moe_sum + part
    for s in range(depth):
        for a in range(2):
            if (s, a) != (0, 0):
                homes[s, a].wait_recv()
            at = s * 2 + a
            moe_sum = moe_sum + weights[:, at : at + 1] * returned[s, a].astype(jnp.float32)
    out[...] = moe_sum.astype(jnp.bfloat16)
    for cp in pending:
        cp.wait_send()


def moe_fused(normed, routes, route_weights, expert_gate, expert_up, expert_down, shared_gate, shared_up, shared_down):
    rows, width = normed.shape
    depth = lax.axis_size("ep") // 2
    e = lax.axis_index("ep")
    z, x = e // 2, e % 2
    source = jnp.stack([((z + depth - s) % depth) * 2 + (x + a) % 2 for s in range(depth) for a in range(2)])
    weights = jnp.sum(
        jnp.where(routes[:, :, None] == source[None, None, :], route_weights[:, :, None], 0.0), axis=1
    )
    units, columns = expert_gate.shape[2], expert_down.shape[2]
    tile = units // TILES
    bf = jnp.bfloat16
    vmem = pl.BlockSpec(memory_space=pltpu.VMEM)
    hbm = pl.BlockSpec(memory_space=pl.ANY)
    dma = pltpu.SemaphoreType.DMA
    pairs = (depth, 2)
    flops = 2 * depth * 2 * rows * (2 * width * units + 4 * units * columns)
    return pl.pallas_call(
        functools.partial(moe_kernel, depth),
        out_shape=jax.ShapeDtypeStruct((rows, columns), bf),
        in_specs=[vmem, vmem, hbm, hbm, hbm, vmem, vmem, vmem],
        out_specs=vmem,
        scratch_shapes=[
            pltpu.VMEM(expert_gate.shape[1:], bf),
            pltpu.VMEM(expert_up.shape[1:], bf),
            pltpu.VMEM(expert_down.shape[1:], bf),
            pltpu.VMEM((depth, 2, 2, rows, width // 2), bf),
            pltpu.VMEM((depth, 4, TILES, 2 * rows, tile), bf),
            pltpu.VMEM((depth, 2, rows, columns), bf),
            pltpu.VMEM((depth, 2, rows, columns), bf),
            pltpu.VMEM((4, rows, shared_gate.shape[1]), bf),
            dma((3,)),
            dma((2,)),
            dma((3,)),
            dma((3,)),
        ]
        + [dma(pairs)] * 4
        + [dma((depth, TILES))] * 6
        + [dma(pairs)] * 2,
        compiler_params=pltpu.CompilerParams(
            collective_id=0, has_side_effects=True, vmem_limit_bytes=44 * 1024 * 1024
        ),
        cost_estimate=pl.CostEstimate(flops=flops * 2, bytes_accessed=40_000_000, transcendentals=0),
    )(normed, weights, expert_gate, expert_up, expert_down, shared_gate, shared_up, shared_down)


def moe_general(normed, routes, route_weights, expert_gate, expert_up, expert_down, shared_gate, shared_up, shared_down):
    rows_b, per_row = routes.shape
    model_width = normed.shape[1]
    groups = lax.axis_size("ep")
    capacity = 2 * rows_b * per_row // groups
    flat_expert = routes.reshape(-1)
    owner_row = jnp.arange(rows_b * per_row, dtype=jnp.int32) // per_row
    expert_hits = (flat_expert[:, None] == jnp.arange(groups, dtype=jnp.int32)[None, :]).astype(
        jnp.int32
    )
    slot_rank = jnp.sum((jnp.cumsum(expert_hits, axis=0) - expert_hits) * expert_hits, axis=1)
    slot_index = flat_expert * capacity + slot_rank
    outgoing = (
        jnp.zeros((groups * capacity, model_width), jnp.bfloat16)
        .at[slot_index]
        .set(normed[owner_row])
    )
    outgoing = outgoing.reshape(groups, capacity, model_width)
    slot_share = capacity // lax.axis_size("tp")
    own_slots = lax.dynamic_slice_in_dim(outgoing, lax.axis_index("tp") * slot_share, slot_share, 1)
    partial_rows = lax.all_to_all(own_slots, "ep", split_axis=0, concat_axis=0, tiled=True)
    arrived = lax.all_gather(partial_rows, "tp", axis=1, tiled=True)
    arrived_rows = arrived.reshape(groups * capacity, model_width)
    gate_value = jnp.dot(arrived_rows, expert_gate[0], preferred_element_type=jnp.float32)
    upward = jnp.dot(arrived_rows, expert_up[0], preferred_element_type=jnp.float32)
    expert_hidden = (jax.nn.silu(gate_value) * upward).astype(jnp.bfloat16)
    shared_hidden = (
        jax.nn.silu(jnp.dot(normed, shared_gate, preferred_element_type=jnp.float32))
        * jnp.dot(normed, shared_up, preferred_element_type=jnp.float32)
    ).astype(jnp.bfloat16)
    columns = expert_down.shape[2]
    routed_sum = jnp.dot(
        lax.all_gather(expert_hidden, "tp", axis=1, tiled=True),
        expert_down[0],
        preferred_element_type=jnp.float32,
    )
    shared_sum = jnp.dot(
        lax.all_gather(shared_hidden, "tp", axis=1, tiled=True),
        shared_down,
        preferred_element_type=jnp.float32,
    )
    expert_out = routed_sum.astype(jnp.bfloat16).reshape(groups, capacity, columns)
    returned = lax.all_to_all(expert_out, "ep", split_axis=0, concat_axis=0, tiled=True).reshape(
        groups * capacity, columns
    )
    picked = returned[slot_index].astype(jnp.float32) * route_weights.reshape(-1)[:, None]
    moe_sum = jnp.sum(picked.reshape(rows_b, per_row, columns), axis=1) + shared_sum
    return moe_sum.astype(jnp.bfloat16)


def body(
    conv_value,
    conv_gate,
    conv_taps,
    norm_gain,
    norm_shift,
    conv_out_weight,
    moe_input,
    moe_gain,
    routes,
    route_weights,
    expert_gate,
    expert_up,
    expert_down,
    shared_gate,
    shared_up,
    shared_down,
):
    tap_count = conv_taps.shape[0]
    rows_a = conv_value.shape[0]
    glu_rows = (
        conv_value.astype(jnp.float32) * jax.nn.sigmoid(conv_gate.astype(jnp.float32))
    ).astype(jnp.bfloat16)
    before = from_behind(glu_rows[rows_a - (tap_count - 1) :], "ep", 1)
    padded = jnp.concatenate([before, glu_rows], axis=0)
    filtered = jnp.zeros(glu_rows.shape, jnp.float32)
    for offset in range(tap_count):
        filtered = filtered + conv_taps[offset] * padded[offset : offset + rows_a].astype(
            jnp.float32
        )
    row_total, squares = lax.psum(
        (jnp.sum(filtered, axis=1), jnp.sum(filtered * filtered, axis=1)), "tp"
    )
    channels = conv_out_weight.shape[0]
    row_mean = row_total / channels
    row_square = squares / channels
    scaled = (filtered - row_mean[:, None]) * lax.rsqrt(row_square - row_mean * row_mean + 1e-05)[
        :, None
    ]
    conv_hidden = jax.nn.silu(scaled * norm_gain + norm_shift).astype(jnp.bfloat16)
    conv_sum = jnp.dot(
        lax.all_gather(conv_hidden, "tp", axis=1, tiled=True),
        conv_out_weight,
        preferred_element_type=jnp.float32,
    )
    conv_result = conv_sum.astype(jnp.bfloat16)
    inputs = moe_input.astype(jnp.float32)
    normed = (
        inputs * lax.rsqrt(jnp.mean(inputs * inputs, axis=1, keepdims=True) + 1e-06) * moe_gain
    ).astype(jnp.bfloat16)
    dense = lax.axis_size("tp") == 4 and lax.axis_size("ep") in (2, 4, 8)
    moe = moe_fused if dense else moe_general
    moe_result = moe(
        normed, routes, route_weights, expert_gate, expert_up, expert_down, shared_gate, shared_up, shared_down
    )
    return (conv_result, moe_result)


def solution(mesh):
    return jax.shard_map(
        body,
        mesh=mesh,
        in_specs=(
            P("ep", "tp"),
            P("ep", "tp"),
            P(None, "tp"),
            P("tp"),
            P("tp"),
            P(None, "tp"),
            P("ep", None),
            P(),
            P("ep", None),
            P("ep", None),
            P("ep", None, "tp"),
            P("ep", None, "tp"),
            P("ep", None, "tp"),
            P(None, "tp"),
            P(None, "tp"),
            P(None, "tp"),
        ),
        out_specs=(P("ep", "tp"), P("ep", "tp")),
        check_vma=False,
    )
```

```python
import functools

import jax
import jax.numpy as jnp
from jax import lax
from jax.experimental import pallas as pl
from jax.experimental.pallas import tpu as pltpu
from jax.sharding import PartitionSpec as P

MESH = pl.DeviceIdType.MESH
TILES = 2
CHUNK = 64


def from_behind(value, axis, steps):
    count = lax.axis_size(axis)
    initial, last = (max(0, -steps), min(count, count - steps))
    return lax.ppermute(value, axis, [(source, source + steps) for source in range(initial, last)])


def silu(v):
    return v / (1.0 + jnp.exp(-v))


def moe_kernel(
    depth,
    normed,
    weights,
    gate_hbm,
    up_hbm,
    down_hbm,
    sgate_hbm,
    sup_hbm,
    sdown_hbm,
    value_hbm,
    cgate_hbm,
    cweight_hbm,
    taps,
    gain,
    shift,
    conv_out,
    out,
    sgate,
    sup,
    sdown,
    value,
    cgate,
    cweight,
    padded,
    filtered,
    stats,
    tail,
    halo,
    rowsums,
    chidden,
    gate,
    up,
    down,
    tokens,
    hidden,
    returned,
    outgoing,
    shidden,
    load_sem,
    own_sem,
    ssend,
    srecv,
    tsend,
    trecv,
    fsend,
    frecv,
    ysend,
    yrecv,
    psend,
    precv,
    gsend,
    grecv,
    rsend,
    rrecv,
    msend,
    mrecv,
    csend,
    crecv,
):
    e = lax.axis_index("ep")
    q = lax.axis_index("tp")
    z, x = e // 2, e % 2
    y, c = q // 2, q % 2
    sister = (e, y * 2 + (1 - c))
    across = (e, (1 - y) * 2 + c)
    beside = (z * 2 + (1 - x), q)
    rows, width = normed.shape
    half = width // 2
    far = (1 - y) * 2 + c

    def home(s, a):
        return (((z + s) % depth) * 2 + (x if a == 0 else 1 - x), q)

    def copy(src, dst, send, recv, device):
        return pltpu.make_async_remote_copy(
            src_ref=src, dst_ref=dst, send_sem=send, recv_sem=recv, device_id=device, device_id_type=MESH
        )

    loads = [
        pltpu.make_async_copy(src, dst, load_sem.at[i])
        for i, (src, dst) in enumerate(
            (
                (value_hbm, value),
                (cgate_hbm, cgate),
                (sgate_hbm, sgate),
                (sup_hbm, sup),
                (gate_hbm.at[0], gate),
                (up_hbm.at[0], up),
                (cweight_hbm, cweight),
                (down_hbm.at[0], down),
                (sdown_hbm, sdown),
            )
        )
    ]
    for load in loads:
        load.start()
    own = [
        pltpu.make_async_copy(normed.at[:, h * half : (h + 1) * half], tokens.at[0, h, 0], own_sem.at[h])
        for h in range(2)
    ]
    for load in own:
        load.start()

    peers = [home(s, a) for s in range(depth) for a in range(2) if (s, a) != (0, 0)]
    peers += [(e, (q + k) % 4) for k in range(1, 4)]
    barrier = pltpu.get_barrier_semaphore()
    for peer in peers:
        pl.semaphore_signal(barrier, inc=1, device_id=peer, device_id_type=MESH)
    pl.semaphore_wait(barrier, len(peers))

    pending = []

    def launch(cp):
        cp.start()
        pending.append(cp)
        return cp

    for load in own:
        load.wait()
    mine = tokens.at[0, c, 0]
    arrive = {}
    arrive[0, 1] = launch(copy(mine, tokens.at[0, c, 1], tsend.at[0, 1], trecv.at[0, 1], beside))
    for s in range(1, depth):
        target = (((z + depth - s) % depth) * 2 + x, q)
        arrive[s, 0] = launch(copy(mine, tokens.at[s, c, 0], tsend.at[s, 0], trecv.at[s, 0], target))

    rows_a, channels = value.shape
    tap_count, edge = taps.shape[0], halo.shape[0]
    lead = edge - (tap_count - 1)
    chunks = rows_a // CHUNK

    def chunk_of(i):
        return pl.multiple_of(i * CHUNK, CHUNK)

    def glu(i, carry):
        at = pl.ds(chunk_of(i), CHUNK)
        gated = value[at, :].astype(jnp.float32) * (1.0 / (1.0 + jnp.exp(-cgate[at, :].astype(jnp.float32))))
        rounded = gated.astype(jnp.bfloat16).astype(jnp.float32)
        padded[pl.ds(pl.multiple_of(i * CHUNK + edge, 8), CHUNK), :] = rounded
        return carry

    loads[0].wait()
    loads[1].wait()
    lax.fori_loop(0, chunks, glu, 0)
    tail[...] = padded[rows_a:, :].astype(jnp.bfloat16)
    count = 2 * depth
    edge_copy = launch(copy(tail, halo, csend.at[0], crecv.at[0], ((e + 1) % count, q)))

    loads[2].wait()
    loads[3].wait()
    shared_gate = jnp.dot(normed[...], sgate[...], preferred_element_type=jnp.float32)
    shared_up = jnp.dot(normed[...], sup[...], preferred_element_type=jnp.float32)
    shidden[q] = (silu(shared_gate) * shared_up).astype(jnp.bfloat16)

    edge_copy.wait_recv()
    padded[0:edge, :] = jnp.where(e == 0, 0.0, halo[...].astype(jnp.float32))
    lane = lax.broadcasted_iota(jnp.int32, (CHUNK, 128), 1)

    def convolve(i, carry):
        start = chunk_of(i)
        at = pl.ds(start, CHUNK)
        sums, squares = jnp.zeros((CHUNK, 128), jnp.float32), jnp.zeros((CHUNK, 128), jnp.float32)
        for column in range(0, channels, 128):
            cols = slice(column, column + 128)
            window = padded[pl.ds(start, CHUNK + edge), cols]
            total = jnp.zeros((CHUNK, 128), jnp.float32)
            for b in range(8):
                size = CHUNK + (8 if b else 0)
                part = None
                for a in range(edge // 8 + 1):
                    j = 8 * a + b - lead
                    if 0 <= j < tap_count:
                        term = taps[j : j + 1, cols] * window[8 * a : 8 * a + size]
                        part = term if part is None else part + term
                if b:
                    part = pltpu.roll(part, size - b, 0)[:CHUNK]
                total = total + part
            filtered[at, cols] = total
            sums = sums + total
            squares = squares + total * total
        row_sum = jnp.sum(sums, axis=1, keepdims=True)
        row_squares = jnp.sum(squares, axis=1, keepdims=True)
        stats[at, :] = jnp.where(lane == 0, row_sum, jnp.where(lane == 1, row_squares, 0.0))
        return carry

    lax.fori_loop(0, chunks, convolve, 0)
    rowsums[q] = stats[...].T[:8]
    mcopies = [
        launch(copy(rowsums.at[q], rowsums.at[q], msend.at[k - 1], mrecv.at[k - 1], (e, (q + k) % 4)))
        for k in range(1, 4)
    ]

    swapped = {}

    def pass_on(s, a):
        arrive[s, a].wait_recv()
        block = tokens.at[s, c, a]
        if a == 0:
            arrive[s, 1] = launch(copy(block, tokens.at[s, c, 1], tsend.at[s, 1], trecv.at[s, 1], beside))
        swapped[s, a] = launch(copy(block, tokens.at[s, c, a], fsend.at[s, a], frecv.at[s, a], sister))

    tile = hidden.shape[4]
    ycopies, pcopies = {}, {}

    def first(s):
        for t in range(TILES):
            cols = slice(t * tile, (t + 1) * tile)

            def product(weight):
                total = None
                for h in range(2):
                    block = tokens[s, h].reshape(2 * rows, half)
                    part = jnp.dot(block, weight[h * half : (h + 1) * half, cols], preferred_element_type=jnp.float32)
                    total = part if total is None else total + part
                return total

            hidden[s, q, t] = (silu(product(gate)) * product(up)).astype(jnp.bfloat16)
            block = hidden.at[s, q, t]
            ycopies[s, t] = launch(copy(block, hidden.at[s, q, t], ysend.at[s, t], yrecv.at[s, t], across))
            pcopies[s, t] = launch(copy(block, hidden.at[s, q, t], psend.at[s, t], precv.at[s, t], sister))

    pass_on(0, 1)
    pass_on(1, 0)
    swapped[0, 1].wait_recv()
    loads[4].wait()
    loads[5].wait()
    first(0)

    for cp in mcopies:
        cp.wait_recv()
    whole = rowsums[0] + rowsums[1] + rowsums[2] + rowsums[3]
    stats[...] = jnp.concatenate([whole, jnp.zeros((120, rows_a), jnp.float32)], axis=0).T
    total_channels = channels * 4

    def normalise(i, carry):
        at = pl.ds(chunk_of(i), CHUNK)
        both = stats[at, :] / total_channels
        mean, square = both[:, 0:1], both[:, 1:2]
        scaled = (filtered[at, :] - mean) * lax.rsqrt(square - mean * mean + 1e-05)
        chidden[q, at, :] = silu(scaled * gain[...] + shift[...]).astype(jnp.bfloat16)
        return carry

    lax.fori_loop(0, chunks, normalise, 0)
    cacross = launch(copy(chidden.at[q], chidden.at[q], csend.at[1], crecv.at[1], across))
    csister = launch(copy(chidden.at[q], chidden.at[q], csend.at[2], crecv.at[2], sister))
    scopies = []
    for k in range(1, 4):
        scopies.append(
            launch(copy(shidden.at[q], shidden.at[q], ssend.at[k - 1], srecv.at[k - 1], (e, (q + k) % 4)))
        )
    for s in range(1, depth):
        if s + 1 < depth:
            pass_on(s + 1, 0)
        pass_on(s, 1)
        swapped[s, 0].wait_recv()
        swapped[s, 1].wait_recv()
        first(s)

    cacross.wait_recv()
    cpassed = launch(copy(chidden.at[far], chidden.at[far], csend.at[3], crecv.at[3], sister))
    csister.wait_recv()
    loads[6].wait()
    cpassed.wait_recv()

    def project(i, carry):
        at = pl.ds(pl.multiple_of(i * 256, 256), 256)
        product = None
        for k in range(4):
            part = jnp.dot(
                chidden[k, at, :],
                cweight[k * channels : (k + 1) * channels, :],
                preferred_element_type=jnp.float32,
            )
            product = part if product is None else product + part
        conv_out[at, :] = product.astype(jnp.bfloat16)
        return carry

    lax.fori_loop(0, rows_a // 256, project, 0)
    loads[7].wait()
    homes = {}
    for s in range(depth):
        forwards = []
        for t in range(TILES):
            ycopies[s, t].wait_recv()
            forwards.append(
                launch(copy(hidden.at[s, far, t], hidden.at[s, far, t], gsend.at[s, t], grecv.at[s, t], sister))
            )
            pcopies[s, t].wait_recv()
        for forward in forwards:
            forward.wait_recv()
        total = None
        for k in range(4):
            for t in range(TILES):
                at = (k * TILES + t) * tile
                part = jnp.dot(hidden[s, k, t], down[at : at + tile, :], preferred_element_type=jnp.float32)
                total = part if total is None else total + part
        for a in range(2):
            piece = total[a * rows : (a + 1) * rows].astype(jnp.bfloat16)
            if (s, a) == (0, 0):
                returned[0, 0] = piece
            else:
                outgoing[s, a] = piece
                homes[s, a] = launch(
                    copy(outgoing.at[s, a], returned.at[s, a], rsend.at[s, a], rrecv.at[s, a], home(s, a))
                )

    for cp in scopies:
        cp.wait_recv()
    loads[8].wait()
    moe_sum = None
    share = shidden.shape[2]
    for k in range(4):
        part = jnp.dot(shidden[k], sdown[k * share : (k + 1) * share, :], preferred_element_type=jnp.float32)
        moe_sum = part if moe_sum is None else moe_sum + part
    for s in range(depth):
        for a in range(2):
            if (s, a) != (0, 0):
                homes[s, a].wait_recv()
            at = s * 2 + a
            moe_sum = moe_sum + weights[:, at : at + 1] * returned[s, a].astype(jnp.float32)
    out[...] = moe_sum.astype(jnp.bfloat16)
    for cp in pending:
        cp.wait_send()


def fused(
    conv, normed, routes, route_weights, expert_gate, expert_up, expert_down, shared_gate, shared_up, shared_down
):
    value, cgate, taps, gain, shift, cweight = conv
    rows_a, channels = value.shape
    edge = -(-(taps.shape[0] - 1) // 8) * 8
    rows, width = normed.shape
    depth = lax.axis_size("ep") // 2
    e = lax.axis_index("ep")
    z, x = e // 2, e % 2
    source = jnp.stack([((z + depth - s) % depth) * 2 + (x + a) % 2 for s in range(depth) for a in range(2)])
    weights = jnp.sum(
        jnp.where(routes[:, :, None] == source[None, None, :], route_weights[:, :, None], 0.0), axis=1
    )
    units, columns = expert_gate.shape[2], expert_down.shape[2]
    tile = units // TILES
    bf = jnp.bfloat16
    vmem = pl.BlockSpec(memory_space=pltpu.VMEM)
    hbm = pl.BlockSpec(memory_space=pl.ANY)
    dma = pltpu.SemaphoreType.DMA
    pairs = (depth, 2)
    flops = 2 * depth * 2 * rows * (2 * width * units + 4 * units * columns)
    return pl.pallas_call(
        functools.partial(moe_kernel, depth),
        out_shape=(
            jax.ShapeDtypeStruct((rows_a, cweight.shape[1]), bf),
            jax.ShapeDtypeStruct((rows, columns), bf),
        ),
        in_specs=[vmem] * 2 + [hbm] * 9 + [vmem] * 3,
        out_specs=(vmem, vmem),
        scratch_shapes=[
            pltpu.VMEM(shared_gate.shape, bf),
            pltpu.VMEM(shared_up.shape, bf),
            pltpu.VMEM(shared_down.shape, bf),
            pltpu.VMEM(value.shape, bf),
            pltpu.VMEM(cgate.shape, bf),
            pltpu.VMEM(cweight.shape, bf),
            pltpu.VMEM((rows_a + edge, channels), jnp.float32),
            pltpu.VMEM((rows_a, channels), jnp.float32),
            pltpu.VMEM((rows_a, 128), jnp.float32),
            pltpu.VMEM((edge, channels), bf),
            pltpu.VMEM((edge, channels), bf),
            pltpu.VMEM((4, 8, rows_a), jnp.float32),
            pltpu.VMEM((4, rows_a, channels), bf),
            pltpu.VMEM(expert_gate.shape[1:], bf),
            pltpu.VMEM(expert_up.shape[1:], bf),
            pltpu.VMEM(expert_down.shape[1:], bf),
            pltpu.VMEM((depth, 2, 2, rows, width // 2), bf),
            pltpu.VMEM((depth, 4, TILES, 2 * rows, tile), bf),
            pltpu.VMEM((depth, 2, rows, columns), bf),
            pltpu.VMEM((depth, 2, rows, columns), bf),
            pltpu.VMEM((4, rows, shared_gate.shape[1]), bf),
            dma((9,)),
            dma((2,)),
            dma((3,)),
            dma((3,)),
        ]
        + [dma(pairs)] * 4
        + [dma((depth, TILES))] * 6
        + [dma(pairs)] * 2
        + [dma((3,))] * 2
        + [dma((4,))] * 2,
        compiler_params=pltpu.CompilerParams(
            collective_id=0, has_side_effects=True, vmem_limit_bytes=56 * 1024 * 1024
        ),
        cost_estimate=pl.CostEstimate(flops=flops * 2, bytes_accessed=40_000_000, transcendentals=0),
    )(
        normed,
        weights,
        expert_gate,
        expert_up,
        expert_down,
        shared_gate,
        shared_up,
        shared_down,
        value,
        cgate,
        cweight,
        taps,
        gain.reshape(1, -1),
        shift.reshape(1, -1),
    )


def moe_general(normed, routes, route_weights, expert_gate, expert_up, expert_down, shared_gate, shared_up, shared_down):
    rows_b, per_row = routes.shape
    model_width = normed.shape[1]
    groups = lax.axis_size("ep")
    capacity = 2 * rows_b * per_row // groups
    flat_expert = routes.reshape(-1)
    owner_row = jnp.arange(rows_b * per_row, dtype=jnp.int32) // per_row
    expert_hits = (flat_expert[:, None] == jnp.arange(groups, dtype=jnp.int32)[None, :]).astype(
        jnp.int32
    )
    slot_rank = jnp.sum((jnp.cumsum(expert_hits, axis=0) - expert_hits) * expert_hits, axis=1)
    slot_index = flat_expert * capacity + slot_rank
    outgoing = (
        jnp.zeros((groups * capacity, model_width), jnp.bfloat16)
        .at[slot_index]
        .set(normed[owner_row])
    )
    outgoing = outgoing.reshape(groups, capacity, model_width)
    slot_share = capacity // lax.axis_size("tp")
    own_slots = lax.dynamic_slice_in_dim(outgoing, lax.axis_index("tp") * slot_share, slot_share, 1)
    partial_rows = lax.all_to_all(own_slots, "ep", split_axis=0, concat_axis=0, tiled=True)
    arrived = lax.all_gather(partial_rows, "tp", axis=1, tiled=True)
    arrived_rows = arrived.reshape(groups * capacity, model_width)
    gate_value = jnp.dot(arrived_rows, expert_gate[0], preferred_element_type=jnp.float32)
    upward = jnp.dot(arrived_rows, expert_up[0], preferred_element_type=jnp.float32)
    expert_hidden = (jax.nn.silu(gate_value) * upward).astype(jnp.bfloat16)
    shared_hidden = (
        jax.nn.silu(jnp.dot(normed, shared_gate, preferred_element_type=jnp.float32))
        * jnp.dot(normed, shared_up, preferred_element_type=jnp.float32)
    ).astype(jnp.bfloat16)
    columns = expert_down.shape[2]
    routed_sum = jnp.dot(
        lax.all_gather(expert_hidden, "tp", axis=1, tiled=True),
        expert_down[0],
        preferred_element_type=jnp.float32,
    )
    shared_sum = jnp.dot(
        lax.all_gather(shared_hidden, "tp", axis=1, tiled=True),
        shared_down,
        preferred_element_type=jnp.float32,
    )
    expert_out = routed_sum.astype(jnp.bfloat16).reshape(groups, capacity, columns)
    returned = lax.all_to_all(expert_out, "ep", split_axis=0, concat_axis=0, tiled=True).reshape(
        groups * capacity, columns
    )
    picked = returned[slot_index].astype(jnp.float32) * route_weights.reshape(-1)[:, None]
    moe_sum = jnp.sum(picked.reshape(rows_b, per_row, columns), axis=1) + shared_sum
    return moe_sum.astype(jnp.bfloat16)


def conv_general(conv_value, conv_gate, conv_taps, norm_gain, norm_shift, conv_out_weight):
    tap_count = conv_taps.shape[0]
    rows_a = conv_value.shape[0]
    glu_rows = (
        conv_value.astype(jnp.float32) * jax.nn.sigmoid(conv_gate.astype(jnp.float32))
    ).astype(jnp.bfloat16)
    before = from_behind(glu_rows[rows_a - (tap_count - 1) :], "ep", 1)
    padded = jnp.concatenate([before, glu_rows], axis=0)
    filtered = jnp.zeros(glu_rows.shape, jnp.float32)
    for offset in range(tap_count):
        filtered = filtered + conv_taps[offset] * padded[offset : offset + rows_a].astype(
            jnp.float32
        )
    row_total, squares = lax.psum(
        (jnp.sum(filtered, axis=1), jnp.sum(filtered * filtered, axis=1)), "tp"
    )
    channels = conv_out_weight.shape[0]
    row_mean = row_total / channels
    row_square = squares / channels
    scaled = (filtered - row_mean[:, None]) * lax.rsqrt(row_square - row_mean * row_mean + 1e-05)[
        :, None
    ]
    conv_hidden = jax.nn.silu(scaled * norm_gain + norm_shift).astype(jnp.bfloat16)
    conv_sum = jnp.dot(
        lax.all_gather(conv_hidden, "tp", axis=1, tiled=True),
        conv_out_weight,
        preferred_element_type=jnp.float32,
    )
    return conv_sum.astype(jnp.bfloat16)


def body(
    conv_value,
    conv_gate,
    conv_taps,
    norm_gain,
    norm_shift,
    conv_out_weight,
    moe_input,
    moe_gain,
    routes,
    route_weights,
    expert_gate,
    expert_up,
    expert_down,
    shared_gate,
    shared_up,
    shared_down,
):
    inputs = moe_input.astype(jnp.float32)
    normed = (
        inputs * lax.rsqrt(jnp.mean(inputs * inputs, axis=1, keepdims=True) + 1e-06) * moe_gain
    ).astype(jnp.bfloat16)
    conv = (conv_value, conv_gate, conv_taps, norm_gain, norm_shift, conv_out_weight)
    moe = (routes, route_weights, expert_gate, expert_up, expert_down, shared_gate, shared_up, shared_down)
    if lax.axis_size("tp") == 4 and lax.axis_size("ep") in (2, 4, 8):
        return fused(conv, normed, *moe)
    return (conv_general(*conv), moe_general(normed, *moe))


def solution(mesh):
    return jax.shard_map(
        body,
        mesh=mesh,
        in_specs=(
            P("ep", "tp"),
            P("ep", "tp"),
            P(None, "tp"),
            P("tp"),
            P("tp"),
            P(None, "tp"),
            P("ep", None),
            P(),
            P("ep", None),
            P("ep", None),
            P("ep", None, "tp"),
            P("ep", None, "tp"),
            P("ep", None, "tp"),
            P(None, "tp"),
            P(None, "tp"),
            P(None, "tp"),
        ),
        out_specs=(P("ep", "tp"), P("ep", "tp")),
        check_vma=False,
    )
```

```python
import functools

import jax
import jax.numpy as jnp
from jax import lax
from jax.experimental import pallas as pl
from jax.experimental.pallas import tpu as pltpu
from jax.sharding import PartitionSpec as P

MESH = pl.DeviceIdType.MESH
TILES = 2
CHUNK = 64


def from_behind(value, axis, steps):
    count = lax.axis_size(axis)
    initial, last = (max(0, -steps), min(count, count - steps))
    return lax.ppermute(value, axis, [(source, source + steps) for source in range(initial, last)])


def silu(v):
    return v / (1.0 + jnp.exp(-v))


def moe_kernel(
    depth,
    normed,
    weights,
    gate_hbm,
    up_hbm,
    down_hbm,
    sgate_hbm,
    sup_hbm,
    sdown_hbm,
    value_hbm,
    cgate_hbm,
    cweight_hbm,
    taps,
    gain,
    shift,
    conv_out,
    out,
    sgate,
    sup,
    sdown,
    value,
    cgate,
    cweight,
    padded,
    filtered,
    stats,
    tail,
    halo,
    rowsums,
    chidden,
    gate,
    up,
    down,
    tokens,
    hidden,
    returned,
    outgoing,
    shidden,
    load_sem,
    own_sem,
    ssend,
    srecv,
    tsend,
    trecv,
    fsend,
    frecv,
    ysend,
    yrecv,
    psend,
    precv,
    gsend,
    grecv,
    rsend,
    rrecv,
    msend,
    mrecv,
    csend,
    crecv,
):
    e = lax.axis_index("ep")
    q = lax.axis_index("tp")
    z, x = e // 2, e % 2
    y, c = q // 2, q % 2
    sister = (e, y * 2 + (1 - c))
    across = (e, (1 - y) * 2 + c)
    beside = (z * 2 + (1 - x), q)
    rows, width = normed.shape
    half = width // 2
    far = (1 - y) * 2 + c

    def home(s, a):
        return (((z + s) % depth) * 2 + (x if a == 0 else 1 - x), q)

    def copy(src, dst, send, recv, device):
        return pltpu.make_async_remote_copy(
            src_ref=src, dst_ref=dst, send_sem=send, recv_sem=recv, device_id=device, device_id_type=MESH
        )

    loads = [
        pltpu.make_async_copy(src, dst, load_sem.at[i])
        for i, (src, dst) in enumerate(
            (
                (value_hbm, value),
                (cgate_hbm, cgate),
                (sgate_hbm, sgate),
                (sup_hbm, sup),
                (gate_hbm.at[0], gate),
                (up_hbm.at[0], up),
                (cweight_hbm, cweight),
                (down_hbm.at[0], down),
                (sdown_hbm, sdown),
            )
        )
    ]
    for load in loads:
        load.start()
    own = [
        pltpu.make_async_copy(normed.at[:, h * half : (h + 1) * half], tokens.at[0, h, 0], own_sem.at[h])
        for h in range(2)
    ]
    for load in own:
        load.start()

    peers = [home(s, a) for s in range(depth) for a in range(2) if (s, a) != (0, 0)]
    peers += [(e, (q + k) % 4) for k in range(1, 4)]
    barrier = pltpu.get_barrier_semaphore()
    for peer in peers:
        pl.semaphore_signal(barrier, inc=1, device_id=peer, device_id_type=MESH)
    pl.semaphore_wait(barrier, len(peers))

    pending = []

    def launch(cp):
        cp.start()
        pending.append(cp)
        return cp

    for load in own:
        load.wait()
    mine = tokens.at[0, c, 0]
    arrive = {}
    arrive[0, 1] = launch(copy(mine, tokens.at[0, c, 1], tsend.at[0, 1], trecv.at[0, 1], beside))
    for s in range(1, depth):
        target = (((z + depth - s) % depth) * 2 + x, q)
        arrive[s, 0] = launch(copy(mine, tokens.at[s, c, 0], tsend.at[s, 0], trecv.at[s, 0], target))

    rows_a, channels = value.shape
    tap_count, edge = taps.shape[0], halo.shape[0]
    lead = edge - (tap_count - 1)
    chunks = rows_a // CHUNK

    def chunk_of(i):
        return pl.multiple_of(i * CHUNK, CHUNK)

    def glu(i, carry):
        at = pl.ds(chunk_of(i), CHUNK)
        gated = value[at, :].astype(jnp.float32) * (1.0 / (1.0 + jnp.exp(-cgate[at, :].astype(jnp.float32))))
        rounded = gated.astype(jnp.bfloat16).astype(jnp.float32)
        padded[pl.ds(pl.multiple_of(i * CHUNK + edge, 8), CHUNK), :] = rounded
        return carry

    loads[0].wait()
    loads[1].wait()
    lax.fori_loop(0, chunks, glu, 0)
    tail[...] = padded[rows_a:, :].astype(jnp.bfloat16)
    count = 2 * depth
    edge_copy = launch(copy(tail, halo, csend.at[0], crecv.at[0], ((e + 1) % count, q)))

    loads[2].wait()
    loads[3].wait()
    shared_gate = jnp.dot(normed[...], sgate[...], preferred_element_type=jnp.float32)
    shared_up = jnp.dot(normed[...], sup[...], preferred_element_type=jnp.float32)
    shidden[q] = (silu(shared_gate) * shared_up).astype(jnp.bfloat16)

    swapped = {}

    def pass_on(s, a):
        arrive[s, a].wait_recv()
        block = tokens.at[s, c, a]
        if a == 0:
            arrive[s, 1] = launch(copy(block, tokens.at[s, c, 1], tsend.at[s, 1], trecv.at[s, 1], beside))
        swapped[s, a] = launch(copy(block, tokens.at[s, c, a], fsend.at[s, a], frecv.at[s, a], sister))

    tile = hidden.shape[4]
    ycopies, pcopies = {}, {}

    def first(s):
        for t in range(TILES):
            cols = slice(t * tile, (t + 1) * tile)

            def product(weight):
                total = None
                for h in range(2):
                    block = tokens[s, h].reshape(2 * rows, half)
                    part = jnp.dot(block, weight[h * half : (h + 1) * half, cols], preferred_element_type=jnp.float32)
                    total = part if total is None else total + part
                return total

            hidden[s, q, t] = (silu(product(gate)) * product(up)).astype(jnp.bfloat16)
            block = hidden.at[s, q, t]
            ycopies[s, t] = launch(copy(block, hidden.at[s, q, t], ysend.at[s, t], yrecv.at[s, t], across))
            pcopies[s, t] = launch(copy(block, hidden.at[s, q, t], psend.at[s, t], precv.at[s, t], sister))

    pass_on(0, 1)
    pass_on(1, 0)
    swapped[0, 1].wait_recv()
    loads[4].wait()
    loads[5].wait()
    first(0)

    edge_copy.wait_recv()
    padded[0:edge, :] = jnp.where(e == 0, 0.0, halo[...].astype(jnp.float32))
    lane = lax.broadcasted_iota(jnp.int32, (CHUNK, 128), 1)

    def convolve(i, carry):
        start = chunk_of(i)
        at = pl.ds(start, CHUNK)
        sums, squares = jnp.zeros((CHUNK, 128), jnp.float32), jnp.zeros((CHUNK, 128), jnp.float32)
        for column in range(0, channels, 128):
            cols = slice(column, column + 128)
            window = padded[pl.ds(start, CHUNK + edge), cols]
            total = jnp.zeros((CHUNK, 128), jnp.float32)
            for b in range(8):
                size = CHUNK + (8 if b else 0)
                part = None
                for a in range(edge // 8 + 1):
                    j = 8 * a + b - lead
                    if 0 <= j < tap_count:
                        term = taps[j : j + 1, cols] * window[8 * a : 8 * a + size]
                        part = term if part is None else part + term
                if b:
                    part = pltpu.roll(part, size - b, 0)[:CHUNK]
                total = total + part
            filtered[at, cols] = total
            sums = sums + total
            squares = squares + total * total
        row_sum = jnp.sum(sums, axis=1, keepdims=True)
        row_squares = jnp.sum(squares, axis=1, keepdims=True)
        stats[at, :] = jnp.where(lane == 0, row_sum, jnp.where(lane == 1, row_squares, 0.0))
        return carry

    lax.fori_loop(0, chunks, convolve, 0)
    rowsums[q] = stats[...].T[:8]
    mcopies = [
        launch(copy(rowsums.at[q], rowsums.at[q], msend.at[k - 1], mrecv.at[k - 1], (e, (q + k) % 4)))
        for k in range(1, 4)
    ]

    scopies = []
    for k in range(1, 4):
        scopies.append(
            launch(copy(shidden.at[q], shidden.at[q], ssend.at[k - 1], srecv.at[k - 1], (e, (q + k) % 4)))
        )
    for s in range(1, depth):
        if s + 1 < depth:
            pass_on(s + 1, 0)
        pass_on(s, 1)
        swapped[s, 0].wait_recv()
        swapped[s, 1].wait_recv()
        first(s)
        if s == 1:
            for cp in mcopies:
                cp.wait_recv()
            whole = rowsums[0] + rowsums[1] + rowsums[2] + rowsums[3]
            stats[...] = jnp.concatenate([whole, jnp.zeros((120, rows_a), jnp.float32)], axis=0).T
            total_channels = channels * 4

            def normalise(i, carry):
                at = pl.ds(chunk_of(i), CHUNK)
                both = stats[at, :] / total_channels
                mean, square = both[:, 0:1], both[:, 1:2]
                scaled = (filtered[at, :] - mean) * lax.rsqrt(square - mean * mean + 1e-05)
                chidden[q, at, :] = silu(scaled * gain[...] + shift[...]).astype(jnp.bfloat16)
                return carry

            lax.fori_loop(0, chunks, normalise, 0)
            cacross = launch(copy(chidden.at[q], chidden.at[q], csend.at[1], crecv.at[1], across))
            csister = launch(copy(chidden.at[q], chidden.at[q], csend.at[2], crecv.at[2], sister))

    cacross.wait_recv()
    cpassed = launch(copy(chidden.at[far], chidden.at[far], csend.at[3], crecv.at[3], sister))
    csister.wait_recv()
    loads[6].wait()
    cpassed.wait_recv()

    def project(i, carry):
        at = pl.ds(pl.multiple_of(i * 256, 256), 256)
        product = None
        for k in range(4):
            part = jnp.dot(
                chidden[k, at, :],
                cweight[k * channels : (k + 1) * channels, :],
                preferred_element_type=jnp.float32,
            )
            product = part if product is None else product + part
        conv_out[at, :] = product.astype(jnp.bfloat16)
        return carry

    lax.fori_loop(0, rows_a // 256, project, 0)
    loads[7].wait()
    homes = {}
    for s in range(depth):
        forwards = []
        for t in range(TILES):
            ycopies[s, t].wait_recv()
            forwards.append(
                launch(copy(hidden.at[s, far, t], hidden.at[s, far, t], gsend.at[s, t], grecv.at[s, t], sister))
            )
            pcopies[s, t].wait_recv()
        for forward in forwards:
            forward.wait_recv()
        total = None
        for k in range(4):
            for t in range(TILES):
                at = (k * TILES + t) * tile
                part = jnp.dot(hidden[s, k, t], down[at : at + tile, :], preferred_element_type=jnp.float32)
                total = part if total is None else total + part
        for a in range(2):
            piece = total[a * rows : (a + 1) * rows].astype(jnp.bfloat16)
            if (s, a) == (0, 0):
                returned[0, 0] = piece
            else:
                outgoing[s, a] = piece
                homes[s, a] = launch(
                    copy(outgoing.at[s, a], returned.at[s, a], rsend.at[s, a], rrecv.at[s, a], home(s, a))
                )

    for cp in scopies:
        cp.wait_recv()
    loads[8].wait()
    moe_sum = None
    share = shidden.shape[2]
    for k in range(4):
        part = jnp.dot(shidden[k], sdown[k * share : (k + 1) * share, :], preferred_element_type=jnp.float32)
        moe_sum = part if moe_sum is None else moe_sum + part
    for s in range(depth):
        for a in range(2):
            if (s, a) != (0, 0):
                homes[s, a].wait_recv()
            at = s * 2 + a
            moe_sum = moe_sum + weights[:, at : at + 1] * returned[s, a].astype(jnp.float32)
    out[...] = moe_sum.astype(jnp.bfloat16)
    for cp in pending:
        cp.wait_send()


def fused(
    conv, normed, routes, route_weights, expert_gate, expert_up, expert_down, shared_gate, shared_up, shared_down
):
    value, cgate, taps, gain, shift, cweight = conv
    rows_a, channels = value.shape
    edge = -(-(taps.shape[0] - 1) // 8) * 8
    rows, width = normed.shape
    depth = lax.axis_size("ep") // 2
    e = lax.axis_index("ep")
    z, x = e // 2, e % 2
    source = jnp.stack([((z + depth - s) % depth) * 2 + (x + a) % 2 for s in range(depth) for a in range(2)])
    weights = jnp.sum(
        jnp.where(routes[:, :, None] == source[None, None, :], route_weights[:, :, None], 0.0), axis=1
    )
    units, columns = expert_gate.shape[2], expert_down.shape[2]
    tile = units // TILES
    bf = jnp.bfloat16
    vmem = pl.BlockSpec(memory_space=pltpu.VMEM)
    hbm = pl.BlockSpec(memory_space=pl.ANY)
    dma = pltpu.SemaphoreType.DMA
    pairs = (depth, 2)
    flops = 2 * depth * 2 * rows * (2 * width * units + 4 * units * columns)
    return pl.pallas_call(
        functools.partial(moe_kernel, depth),
        out_shape=(
            jax.ShapeDtypeStruct((rows_a, cweight.shape[1]), bf),
            jax.ShapeDtypeStruct((rows, columns), bf),
        ),
        in_specs=[vmem] * 2 + [hbm] * 9 + [vmem] * 3,
        out_specs=(vmem, vmem),
        scratch_shapes=[
            pltpu.VMEM(shared_gate.shape, bf),
            pltpu.VMEM(shared_up.shape, bf),
            pltpu.VMEM(shared_down.shape, bf),
            pltpu.VMEM(value.shape, bf),
            pltpu.VMEM(cgate.shape, bf),
            pltpu.VMEM(cweight.shape, bf),
            pltpu.VMEM((rows_a + edge, channels), jnp.float32),
            pltpu.VMEM((rows_a, channels), jnp.float32),
            pltpu.VMEM((rows_a, 128), jnp.float32),
            pltpu.VMEM((edge, channels), bf),
            pltpu.VMEM((edge, channels), bf),
            pltpu.VMEM((4, 8, rows_a), jnp.float32),
            pltpu.VMEM((4, rows_a, channels), bf),
            pltpu.VMEM(expert_gate.shape[1:], bf),
            pltpu.VMEM(expert_up.shape[1:], bf),
            pltpu.VMEM(expert_down.shape[1:], bf),
            pltpu.VMEM((depth, 2, 2, rows, width // 2), bf),
            pltpu.VMEM((depth, 4, TILES, 2 * rows, tile), bf),
            pltpu.VMEM((depth, 2, rows, columns), bf),
            pltpu.VMEM((depth, 2, rows, columns), bf),
            pltpu.VMEM((4, rows, shared_gate.shape[1]), bf),
            dma((9,)),
            dma((2,)),
            dma((3,)),
            dma((3,)),
        ]
        + [dma(pairs)] * 4
        + [dma((depth, TILES))] * 6
        + [dma(pairs)] * 2
        + [dma((3,))] * 2
        + [dma((4,))] * 2,
        compiler_params=pltpu.CompilerParams(
            collective_id=0, has_side_effects=True, vmem_limit_bytes=56 * 1024 * 1024
        ),
        cost_estimate=pl.CostEstimate(flops=flops * 2, bytes_accessed=40_000_000, transcendentals=0),
    )(
        normed,
        weights,
        expert_gate,
        expert_up,
        expert_down,
        shared_gate,
        shared_up,
        shared_down,
        value,
        cgate,
        cweight,
        taps,
        gain.reshape(1, -1),
        shift.reshape(1, -1),
    )


def moe_general(normed, routes, route_weights, expert_gate, expert_up, expert_down, shared_gate, shared_up, shared_down):
    rows_b, per_row = routes.shape
    model_width = normed.shape[1]
    groups = lax.axis_size("ep")
    capacity = 2 * rows_b * per_row // groups
    flat_expert = routes.reshape(-1)
    owner_row = jnp.arange(rows_b * per_row, dtype=jnp.int32) // per_row
    expert_hits = (flat_expert[:, None] == jnp.arange(groups, dtype=jnp.int32)[None, :]).astype(
        jnp.int32
    )
    slot_rank = jnp.sum((jnp.cumsum(expert_hits, axis=0) - expert_hits) * expert_hits, axis=1)
    slot_index = flat_expert * capacity + slot_rank
    outgoing = (
        jnp.zeros((groups * capacity, model_width), jnp.bfloat16)
        .at[slot_index]
        .set(normed[owner_row])
    )
    outgoing = outgoing.reshape(groups, capacity, model_width)
    slot_share = capacity // lax.axis_size("tp")
    own_slots = lax.dynamic_slice_in_dim(outgoing, lax.axis_index("tp") * slot_share, slot_share, 1)
    partial_rows = lax.all_to_all(own_slots, "ep", split_axis=0, concat_axis=0, tiled=True)
    arrived = lax.all_gather(partial_rows, "tp", axis=1, tiled=True)
    arrived_rows = arrived.reshape(groups * capacity, model_width)
    gate_value = jnp.dot(arrived_rows, expert_gate[0], preferred_element_type=jnp.float32)
    upward = jnp.dot(arrived_rows, expert_up[0], preferred_element_type=jnp.float32)
    expert_hidden = (jax.nn.silu(gate_value) * upward).astype(jnp.bfloat16)
    shared_hidden = (
        jax.nn.silu(jnp.dot(normed, shared_gate, preferred_element_type=jnp.float32))
        * jnp.dot(normed, shared_up, preferred_element_type=jnp.float32)
    ).astype(jnp.bfloat16)
    columns = expert_down.shape[2]
    routed_sum = jnp.dot(
        lax.all_gather(expert_hidden, "tp", axis=1, tiled=True),
        expert_down[0],
        preferred_element_type=jnp.float32,
    )
    shared_sum = jnp.dot(
        lax.all_gather(shared_hidden, "tp", axis=1, tiled=True),
        shared_down,
        preferred_element_type=jnp.float32,
    )
    expert_out = routed_sum.astype(jnp.bfloat16).reshape(groups, capacity, columns)
    returned = lax.all_to_all(expert_out, "ep", split_axis=0, concat_axis=0, tiled=True).reshape(
        groups * capacity, columns
    )
    picked = returned[slot_index].astype(jnp.float32) * route_weights.reshape(-1)[:, None]
    moe_sum = jnp.sum(picked.reshape(rows_b, per_row, columns), axis=1) + shared_sum
    return moe_sum.astype(jnp.bfloat16)


def conv_general(conv_value, conv_gate, conv_taps, norm_gain, norm_shift, conv_out_weight):
    tap_count = conv_taps.shape[0]
    rows_a = conv_value.shape[0]
    glu_rows = (
        conv_value.astype(jnp.float32) * jax.nn.sigmoid(conv_gate.astype(jnp.float32))
    ).astype(jnp.bfloat16)
    before = from_behind(glu_rows[rows_a - (tap_count - 1) :], "ep", 1)
    padded = jnp.concatenate([before, glu_rows], axis=0)
    filtered = jnp.zeros(glu_rows.shape, jnp.float32)
    for offset in range(tap_count):
        filtered = filtered + conv_taps[offset] * padded[offset : offset + rows_a].astype(
            jnp.float32
        )
    row_total, squares = lax.psum(
        (jnp.sum(filtered, axis=1), jnp.sum(filtered * filtered, axis=1)), "tp"
    )
    channels = conv_out_weight.shape[0]
    row_mean = row_total / channels
    row_square = squares / channels
    scaled = (filtered - row_mean[:, None]) * lax.rsqrt(row_square - row_mean * row_mean + 1e-05)[
        :, None
    ]
    conv_hidden = jax.nn.silu(scaled * norm_gain + norm_shift).astype(jnp.bfloat16)
    conv_sum = jnp.dot(
        lax.all_gather(conv_hidden, "tp", axis=1, tiled=True),
        conv_out_weight,
        preferred_element_type=jnp.float32,
    )
    return conv_sum.astype(jnp.bfloat16)


def body(
    conv_value,
    conv_gate,
    conv_taps,
    norm_gain,
    norm_shift,
    conv_out_weight,
    moe_input,
    moe_gain,
    routes,
    route_weights,
    expert_gate,
    expert_up,
    expert_down,
    shared_gate,
    shared_up,
    shared_down,
):
    inputs = moe_input.astype(jnp.float32)
    normed = (
        inputs * lax.rsqrt(jnp.mean(inputs * inputs, axis=1, keepdims=True) + 1e-06) * moe_gain
    ).astype(jnp.bfloat16)
    conv = (conv_value, conv_gate, conv_taps, norm_gain, norm_shift, conv_out_weight)
    moe = (routes, route_weights, expert_gate, expert_up, expert_down, shared_gate, shared_up, shared_down)
    if lax.axis_size("tp") == 4 and lax.axis_size("ep") in (2, 4, 8):
        return fused(conv, normed, *moe)
    return (conv_general(*conv), moe_general(normed, *moe))


def solution(mesh):
    return jax.shard_map(
        body,
        mesh=mesh,
        in_specs=(
            P("ep", "tp"),
            P("ep", "tp"),
            P(None, "tp"),
            P("tp"),
            P("tp"),
            P(None, "tp"),
            P("ep", None),
            P(),
            P("ep", None),
            P("ep", None),
            P("ep", None, "tp"),
            P("ep", None, "tp"),
            P("ep", None, "tp"),
            P(None, "tp"),
            P(None, "tp"),
            P(None, "tp"),
        ),
        out_specs=(P("ep", "tp"), P("ep", "tp")),
        check_vma=False,
    )
```
